512 devices in a mesh: sp: 32 (over z, core), tp: 16 (over y, x).
Axes of the slice: x: 4, y: 4, z: 16, core: 2. Of those that a mesh axis runs over, the one named last changes fastest.
Arguments:
- residual: bfloat16 [6144, 2048], P('sp'), may hold values from -6 to 6
- query_in: bfloat16 [6144, 2048], P('sp', 'tp'), may hold values from -6 to 6
- value_in: bfloat16 [6144, 2048], P('sp', 'tp'), may hold values from -6 to 6
- forget_fwd: bfloat16 [6144, 2048], P('sp', 'tp'), may hold values from -4.5 to 4.5
- forget_bwd: bfloat16 [6144, 2048], P('sp', 'tp'), may hold values from -4.5 to 4.5
- jumps: float32 [16, 6144], P('tp', 'sp'), may hold values from -2.8 to 0
- gate_gap: float32 [2, 2048], P(None, 'tp'), may hold values from 0 to 0.1
- out_gate: bfloat16 [6144, 2048], P('sp', 'tp'), may hold values from -6 to 6
- head_gain: float32 [2048], P('tp'), may hold values from 0.1 to 1.9
- out_weight: bfloat16 [2048, 2048], P('tp'), may hold values from -0.25 to 0.25
- norm_gain: float32 [2048], replicated, may hold values from 0.1 to 1.9
- route_ids: int32 [6144, 4], P('sp'), may hold values from 0 to 31, all different within a row; in each aligned block of 192 rows (0 to 191, 192 to 383, ...) at most 36 rows name the same one
- route_weights: float32 [6144, 4], P('sp'), may hold values from 0.05 to 0.5
- w_gate: bfloat16 [32, 2048, 4096], P('sp', None, 'tp'), may hold values from -0.375 to 0.375
- w_up: bfloat16 [32, 2048, 4096], P('sp', None, 'tp'), may hold values from -0.375 to 0.375
- w_down: bfloat16 [32, 4096, 2048], P('sp', None, 'tp'), may hold values from -0.09375 to 0.09375
Outputs:
- mixed: bfloat16 [6144, 2048], P('sp', 'tp')
The draws below stay inside these ranges and needn't reach their ends.
Inputs may be any that keep to these rules, and one draw needn't show every extreme that they name: `route_ids`: in each aligned block of 192 rows each expert is named by at most 36 rows, and by exactly 36 in some block; each row names 4 different experts.
All inputs are finite; a program needn't handle non-finite values.
Results may differ from the reference program's by a relative error of at most 0.024.
Values may be sent and summed in bfloat16 or wider, within the bound.
A program may use at most 64 MiB of HBM per device.

```python
import math
import jax
import jax.numpy as jnp
import numpy as np
from jax import lax

HEADS = 16
HEAD_DIM = 128
D = 2048
FF = 4096
EXPERTS = 32
TOP = 4
TOK_SP = 192
TOKENS = 6144
CAP = 36
N_SP = 32
N_TP = 16


def draw_gate_gap(key, part):
    head_key, fast_key, slow_key = jax.random.split(jax.random.fold_in(key, 11), 3)
    fast_share = 0.5
    fast_heads = jax.random.uniform(head_key, (2, HEADS, 1), jnp.float32) < fast_share
    fast_gap = jax.random.uniform(fast_key, (2, HEADS, HEAD_DIM), jnp.float32, math.log(0.03), math.log(0.1))
    slow_gap = jax.random.uniform(slow_key, (2, HEADS, HEAD_DIM), jnp.float32, math.log(0.2), 0.0)
    gap_values = jnp.where(fast_heads, jnp.exp(fast_gap), jnp.exp(slow_gap) / TOKENS)
    return gap_values.reshape(2, D).astype(jnp.float32)


def forget_values(key):
    noise_key, level_key = jax.random.split(key)
    noise = jnp.clip(jax.random.normal(noise_key, (TOKENS, D), jnp.float32), -3.0, 3.0)
    levels = jax.random.uniform(level_key, (TOKENS // TOK_SP, 1, HEADS, 1), jnp.float32, -1.5, 1.5)
    shifted = noise.reshape(TOKENS // TOK_SP, TOK_SP, HEADS, HEAD_DIM) + levels
    return shifted.reshape(TOKENS, D).astype(jnp.bfloat16)


def draw_forget_fwd(key, part):
    return forget_values(jax.random.fold_in(key, 21))


def draw_forget_bwd(key, part):
    return forget_values(jax.random.fold_in(key, 22))


def draw_jumps(key, part):
    spot_key, size_key = jax.random.split(jax.random.fold_in(key, 31))
    spots = jax.random.randint(spot_key, (HEADS, 4), 0, TOKENS)
    sizes = jax.random.uniform(size_key, (HEADS, 4), jnp.float32, math.log(0.5), math.log(0.8))
    hits = jnp.arange(TOKENS, dtype=jnp.int32)[None, :, None] == spots[:, None, :]
    return jnp.sum(jnp.where(hits, sizes[:, None, :], 0.0), axis=2).astype(jnp.float32)


def block_scale(stream_key, shape, shards, smallest, high):
    loudness = 1.0
    for dim, blocks in shards:
        heights = jax.random.uniform(jax.random.fold_in(jax.random.fold_in(stream_key, 6), dim), (blocks,), jnp.float32, smallest / len(shards), high / len(shards))
        loudness = loudness * jnp.repeat(jnp.exp(heights), shape[dim] // blocks).reshape((-1,) + (1,) * (len(shape) - 1 - dim))
    return loudness


def shared_out(key, own, number, rows, number_of, top, limit, slope):
    ranking = jax.random.permutation(key, number_of)
    packed, common = shares(number_of, rows * top, limit, slope, True), shares(number_of, rows * top, limit, slope, False)
    places = jnp.arange(number_of)

    def named(tallies, turn):
        used = int((tallies > 0).sum())
        fixed = max(1, used // 4)
        moved = fixed + (places - fixed + turn * (used - fixed)) % max(1, number_of - fixed)
        return jnp.zeros((number_of,), jnp.int32).at[ranking[jnp.where(places < fixed, places, moved)]].set(jnp.asarray(tallies, jnp.int32))

    tallies = jnp.where(number % 4 == 0, named(packed, number // 4), named(common, number - number // 4 - 1))
    mixed = jax.random.permutation(jax.random.fold_in(own, 3), number_of)
    source_of, taker = mixed[0:number_of // 2 * 2:2], mixed[1:number_of // 2 * 2:2]
    slack = jnp.minimum(tallies[source_of] - 1, limit - tallies[taker]) // 2
    slack = jnp.where((source_of == ranking[0]) | (taker == ranking[0]) | (tallies[taker] == 0), 0, jnp.maximum(slack, 0))
    moved = jax.random.randint(jax.random.fold_in(own, 4), (number_of // 2,), 0, 1 << 20) % (slack + 1)
    tallies = tallies.at[source_of].add(-moved).at[taker].add(moved)
    labels = jnp.searchsorted(jnp.cumsum(tallies), jnp.arange(rows * top), side="right").astype(jnp.int32)
    grid = labels.reshape(top, rows).T
    grid = grid[jax.random.permutation(jax.random.fold_in(own, 1), rows)]
    turn = jax.random.randint(jax.random.fold_in(own, 2), (rows, 1), 0, top)
    return jnp.take_along_axis(grid, (jnp.arange(top)[None, :] + turn) % top, axis=1)


def shares(number_of, total, reach, lean, full):
    weights = [(1 << 20) // math.isqrt(grade ** lean) + 1 for grade in range(1, number_of + 1)]
    largest = reach if full else min(reach, max(-(-total // number_of), total * weights[0] // sum(weights)))
    least = 1 if total - largest >= number_of - 1 else 0
    counts, surplus = [largest] + [least] * (number_of - 1), total - largest - least * (number_of - 1)
    while surplus > 0:
        movable = [i for i in range(1, number_of) if counts[i] < largest] or [i for i in range(1, number_of) if counts[i] < reach]
        pool, left = sum([weights[i] for i in movable]), surplus
        for i in movable:
            extra = min(reach - counts[i], max(1, left * weights[i] // pool), surplus)
            counts[i] = counts[i] + extra
            surplus = surplus - extra
    return np.array(counts)


def scatter_about(stream_key, shape, scale, bound, pieces=(), held_as=jnp.bfloat16):
    entries = scale * jax.random.normal(stream_key, shape, jnp.float32)
    if pieces:
        entries = entries * block_scale(stream_key, shape, pieces, -0.22, 0.18)
    return jnp.clip(entries, -bound, bound).astype(held_as)


def setup_inputs(seed: int = 0) -> dict:
    streams_of = jax.random.split(jax.random.key(seed), 17)
    residual = scatter_about(streams_of[0], (TOKENS, D), 1.0, 6.0, ((0, 32),))
    query_in = scatter_about(streams_of[1], (TOKENS, D), 1.0, 6.0, ((0, 32), (1, 16)))
    value_in = scatter_about(streams_of[2], (TOKENS, D), 1.0, 6.0, ((0, 32), (1, 16)))
    forget_fwd = draw_forget_fwd(jax.random.fold_in(streams_of[16], 71), 0)
    forget_bwd = draw_forget_bwd(jax.random.fold_in(streams_of[16], 71), 0)
    jumps = draw_jumps(jax.random.fold_in(streams_of[16], 71), 0)
    gate_gap = draw_gate_gap(jax.random.fold_in(streams_of[16], 71), 0)
    out_gate = scatter_about(streams_of[7], (TOKENS, D), 1.0, 6.0, ((0, 32), (1, 16)))
    head_gain = jnp.clip(1.0 + 0.18 * jax.random.normal(streams_of[8], (D,), jnp.float32), 0.1, 1.9)
    out_weight = scatter_about(streams_of[9], (D, D), (D // 4) ** -0.5, 0.25, ((0, 16),))
    norm_gain = jnp.clip(1.0 + 0.18 * jax.random.normal(streams_of[10], (D,), jnp.float32), 0.1, 1.9)
    route_ids_keys = jax.random.split(jax.random.fold_in(streams_of[11], 1), TOKENS // TOK_SP)
    route_ids_turns = jax.random.permutation(jax.random.fold_in(streams_of[11], 3), TOKENS // TOK_SP)
    route_ids = jax.vmap(lambda own, number: shared_out(jax.random.fold_in(streams_of[11], 2), own, number, TOK_SP, EXPERTS, TOP, CAP, 1))(route_ids_keys, route_ids_turns).reshape((TOKENS, TOP))
    route_weights = jnp.clip(jnp.exp(math.log(0.5) - 2.3025851 * jax.random.uniform(streams_of[12], (TOKENS, TOP), jnp.float32) ** block_scale(streams_of[12], (TOKENS, TOP), ((0, 32),), -0.2, 0.2)), 0.05, 0.5)
    w_gate = scatter_about(streams_of[13], (EXPERTS, D, FF), (D // 8) ** -0.5, 0.375, ((0, 32), (2, 16)))
    w_up = scatter_about(streams_of[14], (EXPERTS, D, FF), (D // 8) ** -0.5, 0.375, ((0, 32), (2, 16)))
    w_down = scatter_about(streams_of[15], (EXPERTS, FF, D), FF ** -0.5, 0.09375, ((0, 32), (2, 16)))
    return dict(residual=residual, query_in=query_in, value_in=value_in, forget_fwd=forget_fwd, forget_bwd=forget_bwd, jumps=jumps, gate_gap=gate_gap, out_gate=out_gate, head_gain=head_gain, out_weight=out_weight, norm_gain=norm_gain, route_ids=route_ids, route_weights=route_weights, w_gate=w_gate, w_up=w_up, w_down=w_down)


highest_precision = lax.Precision.HIGHEST
eps_norm = 1e-06
limit_value = 7.0
alpha_value = 1.702

def recurrence(queries, keys_in, values, logs):

    def advance(current_state, step_items):
        current_query, key_now, value_now, log_now = step_items
        current_state = current_state * jnp.exp(log_now)[:, :, None] + key_now[:, :, None] * value_now[:, None, :]
        return (current_state, jnp.einsum('ob,obs->os', current_query, current_state, precision=highest_precision))
    zero_state = jnp.zeros((queries.shape[1], queries.shape[2], values.shape[2]), jnp.float32)
    unused, outputs = lax.scan(advance, zero_state, (queries, keys_in, values, logs))
    return outputs

def reference(residual, query_in, value_in, forget_fwd, forget_bwd, jumps, gate_gap, out_gate, head_gain, out_weight, norm_gain, route_ids, route_weights, w_gate, w_up, w_down):
    tokens, width = query_in.shape
    head_count = jumps.shape[0]
    head_width = width // head_count

    def by_head(array):
        return array.astype(jnp.float32).reshape(tokens, head_count, head_width)
    queries = jax.nn.silu(by_head(query_in))
    values = by_head(value_in)
    jump_rows = jnp.transpose(jumps)[:, :, None]

    def gate_terms(forget_in, gap):
        key_share = gap.reshape(head_count, head_width) * jax.nn.sigmoid(-by_head(forget_in))
        return (key_share, jnp.log1p(-key_share) + jump_rows)
    keys_fwd, logs_fwd = gate_terms(forget_fwd, gate_gap[0])
    keys_bwd, logs_bwd = gate_terms(forget_bwd, gate_gap[1])
    forward_out = recurrence(queries, keys_fwd, values, logs_fwd)
    backward_out = jnp.flip(recurrence(jnp.flip(queries, 0), jnp.flip(keys_bwd, 0), jnp.flip(values, 0), jnp.flip(logs_bwd, 0)), 0)
    mixed_heads = forward_out + backward_out
    mean_square = lax.optimization_barrier(jnp.mean(mixed_heads * mixed_heads, axis=-1, keepdims=True))
    normed = (mixed_heads * lax.rsqrt(mean_square + eps_norm)).reshape(tokens, width)
    gated = (normed * head_gain * jax.nn.silu(out_gate.astype(jnp.float32))).astype(jnp.bfloat16)
    group_width = width // N_TP
    gated_groups = jnp.transpose(gated.reshape(tokens, N_TP, group_width), (1, 0, 2))
    weight_groups = out_weight.reshape(N_TP, group_width, width)

    def add_group(total, group_items):
        term = jnp.dot(group_items[0], group_items[1], preferred_element_type=jnp.float32).astype(jnp.bfloat16)
        term = lax.optimization_barrier(term)
        return (total + term.astype(jnp.float32), None)
    summed, unused = lax.scan(add_group, jnp.zeros((tokens, width), jnp.float32), (gated_groups, weight_groups))
    stream = (residual.astype(jnp.float32) + summed).astype(jnp.bfloat16)
    stream_f = stream.astype(jnp.float32)
    row_scale = lax.rsqrt(lax.optimization_barrier(jnp.mean(stream_f * stream_f, axis=-1, keepdims=True)) + eps_norm)
    normed_rows = (stream_f * row_scale * norm_gain).astype(jnp.bfloat16)
    block = tokens // N_SP
    group_ids = route_ids.reshape(N_SP, block * TOP)
    one_hot = (group_ids[:, :, None] == jnp.arange(EXPERTS, dtype=jnp.int32)[None, None, :]).astype(jnp.int32)
    slot_rank = lax.optimization_barrier(jnp.sum((jnp.cumsum(one_hot, axis=1) - 1) * one_hot, axis=2))
    group_index = jnp.arange(N_SP, dtype=jnp.int32)[:, None]
    slot_index = (group_ids * (N_SP * CAP) + group_index * CAP + slot_rank).reshape(-1).astype(jnp.int32)
    owner_rows = (jnp.arange(tokens * TOP, dtype=jnp.int32) // TOP).astype(jnp.int32)
    slot_rows = jnp.full((EXPERTS * N_SP * CAP,), tokens, jnp.int32).at[slot_index].set(owner_rows)
    padded_rows = jnp.concatenate([normed_rows, jnp.zeros((1, width), jnp.bfloat16)], axis=0)

    def expert(expert_items):
        rows_index, gate_weight, up_weight, down_weight = expert_items
        rows = padded_rows[rows_index]
        gate_sum = jnp.minimum(jnp.dot(rows, gate_weight, preferred_element_type=jnp.float32), limit_value)
        up_sum = jnp.clip(jnp.dot(rows, up_weight, preferred_element_type=jnp.float32), -limit_value, limit_value)
        active = (gate_sum * jax.nn.sigmoid(alpha_value * gate_sum) * (up_sum + 1.0)).astype(jnp.bfloat16)
        return jnp.dot(active, down_weight, preferred_element_type=jnp.float32).astype(jnp.bfloat16)
    produced = lax.map(expert, (slot_rows.reshape(EXPERTS, N_SP * CAP), w_gate, w_up, w_down))
    picked = produced.reshape(EXPERTS * N_SP * CAP, width)[slot_index].astype(jnp.float32).reshape(tokens, TOP, width)
    moe_out = lax.optimization_barrier(jnp.sum(picked * route_weights[:, :, None], axis=1))
    return (stream_f + moe_out).astype(jnp.bfloat16)
```

```python
import jax
import jax.numpy as jnp
from jax import lax
from jax.experimental import pallas as pl
from jax.experimental.pallas import tpu as pltpu
from jax.sharding import PartitionSpec as P

MESH = pl.DeviceIdType.MESH
HIGH = lax.Precision.HIGHEST
F32 = jnp.float32
BF16 = jnp.bfloat16
NSP = 32
NTP = 16
T = 192
W = 128
CAP = 36
PAD = 48
ROWS = NSP * CAP
SLOTS = NSP * PAD
TILE = 288
EPS = 1e-06
LIMIT = 7.0
ALPHA = 1.702


def iota(shape, dim):
    return lax.broadcasted_iota(jnp.int32, shape, dim)


def nn(a, b, precision=None):
    return jnp.dot(a, b, preferred_element_type=F32, precision=precision)


def nt(a, b, precision=None):
    return lax.dot_general(a, b, (((1,), (1,)), ((), ())), preferred_element_type=F32, precision=precision)


def tn(a, b, precision=None):
    return lax.dot_general(a, b, (((0,), (0,)), ((), ())), preferred_element_type=F32, precision=precision)


def onehot(mask):
    return jnp.where(mask, 1.0, 0.0).astype(BF16)


def split(a):
    high = a.astype(BF16)
    return high, (a - high.astype(F32)).astype(BF16)


def remote(src, dst, send, recv, device):
    return pltpu.make_async_remote_copy(
        src_ref=src, dst_ref=dst, send_sem=send, recv_sem=recv, device_id=device, device_id_type=MESH
    )


class Exchange:
    def __init__(self, axis, size, source, target, send, recv):
        self.axis, self.size, self.source, self.target = axis, size, source, target
        self.send, self.recv = send, recv
        self.me = lax.axis_index(axis)

    def copy(self, d, to, slot):
        return remote(
            self.source(to), self.target(slot), self.send.at[d], self.recv.at[d], {self.axis: to}
        )

    def start(self):
        @pl.loop(1, self.size)
        def _(d):
            to = lax.rem(self.me + d, self.size)
            self.copy(d, to, self.me).start()

    def wait(self):
        @pl.loop(1, self.size)
        def _(d):
            origin = lax.rem(self.me - d + self.size, self.size)
            self.copy(d, origin, origin).wait()


class Torus:
    def __init__(self):
        t = lax.axis_index("tp")
        self.y, self.x = t // 4, lax.rem(t, 4)

    def index(self, along_x):
        return self.x if along_x else self.y

    def device(self, along_x, j):
        return {"tp": self.y * 4 + j if along_x else j * 4 + self.x}


def near(i):
    return lax.rem(i + 1, 4), lax.rem(i + 3, 4), lax.rem(i + 2, 4)


class Gather:
    def __init__(self, torus, ref, rows, base, send, recv, number):
        self.t, self.ref, self.rows, self.base = torus, ref, rows, base
        self.send, self.recv, self.number = send, recv, number

    def view(self, half, stage, j, q):
        piece = self.rows // 4
        rows = pl.ds(self.base + half * (self.rows // 2) + q * piece, piece)
        if (half == 0) == (stage == 0):
            return self.ref.at[self.t.y, j, rows] if stage == 0 else self.ref.at[:, j, rows]
        return self.ref.at[j, self.t.x, rows] if stage == 0 else self.ref.at[j, :, rows]

    def copy(self, half, stage, k, arriving=False):
        along = (half == 0) == (stage == 0)
        i = self.t.index(along)
        p, m, f = near(i)
        up = k < 3
        to = p if up else m
        q = (0, 1, 0, 1, 0, 1)[k]
        if arriving:
            j = (m, m, f, p, p, f)[k]
        else:
            j = (i, i, m, i, i, p)[k]
        ref = self.view(half, stage, j, q)
        n = self.number * 24 + half * 12 + stage * 6 + k
        return remote(ref, ref, self.send.at[n], self.recv.at[n], self.t.device(along, to))

    def begin(self, half, stage):
        for k in (0, 3, 1, 4):
            self.copy(half, stage, k).start()

    def relay(self, half, stage):
        for k, then in ((0, 2), (3, 5)):
            self.copy(half, stage, k, True).wait_recv()
            self.copy(half, stage, then).start()

    def end(self, half, stage):
        for k in (1, 4, 2, 5):
            self.copy(half, stage, k, True).wait_recv()

    def drain(self):
        for half in range(2):
            for stage in range(2):
                for k in range(6):
                    self.copy(half, stage, k).wait_send()

    def run(self):
        for stage in range(2):
            for half in range(2):
                self.begin(half, stage)
            for half in range(2):
                self.relay(half, stage)
            for half in range(2):
                self.end(half, stage)


class Reduce:
    def __init__(self, torus, ref, rows, base, wide, narrow, send, recv, number):
        self.t, self.ref, self.rows, self.base = torus, ref, rows, base
        self.wide, self.narrow, self.send, self.recv, self.number = wide, narrow, send, recv, number

    def along(self, half, stage):
        return (half == 0) != (stage == 0)

    def view(self, half, stage, j, q):
        piece = self.rows // 4
        rows = pl.ds(self.base + half * (self.rows // 2) + q * piece, piece)
        if self.along(half, stage):
            return self.ref.at[self.t.y, j, rows] if stage == 1 else self.ref.at[:, j, rows]
        return self.ref.at[j, self.t.x, rows] if stage == 1 else self.ref.at[j, :, rows]

    def slot(self, half, stage, k):
        n = (self.number * 2 + half) * 6 + k
        return self.wide.at[n] if stage == 0 else self.narrow.at[n]

    def copy(self, half, stage, k):
        along = self.along(half, stage)
        i = self.t.index(along)
        p, m, f = near(i)
        to = p if k < 3 else m
        q = (0, 1, 0, 1, 0, 1)[k]
        j = (f, p, p, f, m, m)[k]
        n = self.number * 24 + half * 12 + stage * 6 + k
        return remote(
            self.view(half, stage, j, q),
            self.slot(half, stage, k),
            self.send.at[n],
            self.recv.at[n],
            self.t.device(along, to),
        )

    def add(self, half, stage, j, q, ks):
        own = self.view(half, stage, j, q)
        refs = [self.slot(half, stage, k) for k in ks]
        if stage == 0:
            @pl.loop(0, 4)
            def _(a):
                total = own[a].astype(F32)
                for ref in refs:
                    total = total + ref[a].astype(F32)
                own[a] = total.astype(BF16)
        else:
            total = own[...].astype(F32)
            for ref in refs:
                total = total + ref[...].astype(F32)
            own[...] = total.astype(BF16)

    def begin(self, half, stage):
        for k in (0, 3, 1, 4):
            self.copy(half, stage, k).start()

    def relay(self, half, stage):
        p, m, f = near(self.t.index(self.along(half, stage)))
        self.copy(half, stage, 0).wait_recv()
        self.add(half, stage, p, 0, (0,))
        self.copy(half, stage, 2).start()
        self.copy(half, stage, 3).wait_recv()
        self.add(half, stage, m, 1, (3,))
        self.copy(half, stage, 5).start()

    def end(self, half, stage):
        i = self.t.index(self.along(half, stage))
        for q, ks in ((0, (2, 4)), (1, (1, 5))):
            for k in ks:
                self.copy(half, stage, k).wait_recv()
            self.add(half, stage, i, q, ks)

    def drain(self):
        for half in range(2):
            for stage in range(2):
                for k in range(6):
                    self.copy(half, stage, k).wait_send()

    def run(self):
        for stage in range(2):
            for half in range(2):
                self.begin(half, stage)
            for half in range(2):
                self.relay(half, stage)
            for half in range(2):
                self.end(half, stage)


def layer(
    residual, query_in, value_in, forget_fwd, forget_bwd, jumps, gate_gap, out_gate, head_gain,
    out_weight, norm_gain, route_ids, route_weights, w_gate, w_up, w_down,
    mixed,
    wg, wu, wd, wo, res, states, got, scanned, answers, carries,
    gat, disp, comb, sent, came, rows, xs, act, part, wide, narrow, outs, back,
    local, zsend, zrecv, tsend, trecv, gsend, grecv, rsend, rrecv,
):
    sp, tp = lax.axis_index("sp"), lax.axis_index("tp")
    torus = Torus()
    y, x = torus.y, torus.x

    barrier = pltpu.get_barrier_semaphore()

    @pl.loop(1, NSP)
    def _(d):
        pl.semaphore_signal(barrier, 1, device_id={"sp": lax.rem(sp + d, NSP)}, device_id_type=MESH)

    @pl.loop(1, NTP)
    def _(d):
        pl.semaphore_signal(barrier, 1, device_id={"tp": lax.rem(tp + d, NTP)}, device_id_type=MESH)

    mine_t = pl.ds(pl.multiple_of(tp * W, W), W)
    own = [
        pltpu.make_async_copy(residual.at[:, mine_t], res, local.at[0]),
        pltpu.make_async_copy(out_weight.at[:, mine_t], wo.at[tp], local.at[1]),
        pltpu.make_async_copy(w_gate.at[0], wg, local.at[2]),
        pltpu.make_async_copy(w_up.at[0], wu, local.at[3]),
        pltpu.make_async_copy(
            w_down.at[0, pl.ds(pl.multiple_of(tp * 256, 256), 256)], wd.at[:, mine_t], local.at[4]
        ),
    ]
    for copy in own:
        copy.start()

    ti, si = iota((T, T), 0), iota((T, T), 1)
    until = jnp.where(si <= ti, 1.0, 0.0)
    before = jnp.where(si < ti, 1.0, 0.0)
    jump = jnp.broadcast_to(jumps[...], (8, T))
    jump_in = nt(until, jump, HIGH)[:, 0:1]
    jump_ex = nt(before, jump, HIGH)[:, 0:1]
    jump_in_row = nt(jump, until, HIGH)[0:1, :]
    jump_ex_row = nt(jump, before, HIGH)[0:1, :]
    jump_all = jump_in_row[:, T - 1 : T]

    raw = query_in[...].astype(F32)
    queries = raw * jax.nn.sigmoid(raw)
    values = value_in[...]

    key_f = gate_gap[0:1, :] * jax.nn.sigmoid(-forget_fwd[...].astype(F32))
    log_f = jnp.log1p(-key_f)
    sum_f = nn(until, log_f, HIGH)
    all_f = sum_f[T - 1 : T, :]
    mid_f = all_f * 0.5
    scores = jnp.where(
        si <= ti,
        nt((queries * jnp.exp(sum_f - mid_f)).astype(BF16), (key_f * jnp.exp(mid_f - sum_f)).astype(BF16))
        * jnp.exp(jnp.minimum(jump_in - jump_in_row, 0.0)),
        0.0,
    )
    decay_f = jnp.exp(all_f + jump_all)
    state_f = tn(values, (key_f * jnp.exp((all_f - sum_f) + (jump_all - jump_in))).astype(BF16))
    reach_f = (queries * jnp.exp(sum_f + jump_in)).astype(BF16)

    key_b = gate_gap[1:2, :] * jax.nn.sigmoid(-forget_bwd[...].astype(F32))
    log_b = jnp.log1p(-key_b)
    sum_b = nn(before, log_b, HIGH)
    all_b = sum_b[T - 1 : T, :] + log_b[T - 1 : T, :]
    mid_b = all_b * 0.5
    scores = scores + jnp.where(
        si >= ti,
        nt((queries * jnp.exp(mid_b - sum_b)).astype(BF16), (key_b * jnp.exp(sum_b - mid_b)).astype(BF16))
        * jnp.exp(jnp.minimum(jump_ex_row - jump_ex, 0.0)),
        0.0,
    )
    decay_b = jnp.exp(all_b + jump_all)
    state_b = tn(values, (key_b * jnp.exp(sum_b + jump_ex)).astype(BF16))
    reach_b = (queries * jnp.exp((all_b - sum_b) + (jump_all - jump_ex))).astype(BF16)
    within = nn(scores.astype(BF16), values)

    i, j = iota((512, 256), 0), iota((512, 256), 1)
    r = i & 15
    place = onehot(((r < 8) & (j == (i >> 4) * 4 + (r & 3) + jnp.where(r < 4, 0, 128))))
    pieces = nn(place, jnp.concatenate([state_f.astype(BF16), state_b.astype(BF16)], axis=0))
    r = iota((512, W), 0) & 15
    for number, decay in ((8, decay_f), (10, decay_b)):
        high, low = split(decay)
        pieces = jnp.where(r == number, high.astype(F32), pieces)
        pieces = jnp.where(r == number + 1, low.astype(F32), pieces)
    states[...] = pieces.astype(BF16)

    pl.semaphore_wait(barrier, NSP + NTP - 2)

    def piece(ref):
        return lambda n: ref.at[pl.ds(pl.multiple_of(n * 16, 16), 16)]

    def slab(ref):
        return lambda n: ref.at[n, pl.ds(0, PAD)]

    there = Exchange("sp", NSP, piece(states), piece(got), zsend.at[0], zrecv.at[0])
    again = Exchange("sp", NSP, piece(answers), piece(carries), zsend.at[1], zrecv.at[1])
    shipped = Exchange("sp", NSP, slab(sent), slab(came), zsend.at[2], zrecv.at[2])
    returned = Exchange("sp", NSP, slab(outs), slab(back), zsend.at[3], zrecv.at[3])
    project = Exchange(
        "tp", NTP, lambda n: out_weight.at[:, pl.ds(pl.multiple_of(n * W, W), W)],
        lambda n: wo.at[n], tsend.at[0], trecv.at[0],
    )
    down = Exchange(
        "tp", NTP, lambda n: w_down.at[0, pl.ds(pl.multiple_of(n * 256, 256), 256)],
        lambda n: wd.at[:, pl.ds(pl.multiple_of(n * W, W), W)], tsend.at[1], trecv.at[1],
    )
    there.start()
    project.start()
    down.start()
    mine_s = pl.ds(pl.multiple_of(sp * 16, 16), 16)
    got[mine_s] = states[mine_s]

    ids = route_ids[...]
    weights = route_weights[...]
    lane = iota((T, W), 1)
    named = jnp.zeros((T, W), F32)
    weighted = jnp.zeros((T, W), F32)
    for n in range(4):
        hit = ids[:, n : n + 1] == lane
        named = named + jnp.where(hit, 1.0, 0.0)
        weighted = weighted + jnp.where(hit, weights[:, n : n + 1], 0.0)
    named16 = named.astype(BF16)
    rank16 = nn(before.astype(BF16), named16).astype(BF16)
    w_high, w_low = split(weighted)
    STEP = 384
    for c in range(SLOTS // STEP):
        slot, e = iota((STEP, W), 0) + c * STEP, iota((STEP, W), 1)
        owns = onehot((slot >= e * PAD) & (slot < e * PAD + PAD))
        number = nt(owns, jnp.broadcast_to(lax.broadcasted_iota(jnp.int32, (8, W), 1).astype(F32), (8, W)).astype(BF16))
        turn = (iota((STEP, 1), 0) + c * STEP).astype(F32) - PAD * number[:, 0:1]
        picked = (nt(owns, named16) > 0.5) & (nt(owns, rank16) == turn)
        disp[c * STEP : (c + 1) * STEP, :] = onehot(picked)

        slot, e = iota((W, STEP), 1) + c * STEP, iota((W, STEP), 0)
        owns = onehot((slot >= e * PAD) & (slot < e * PAD + PAD))
        number = nn(lax.broadcasted_iota(jnp.int32, (8, W), 1).astype(F32).astype(BF16), owns)
        turn = (iota((1, STEP), 1) + c * STEP).astype(F32) - PAD * number[0:1, :]
        picked = (nn(named16, owns) > 0.5) & (nn(rank16, owns) == turn)
        comb[0, :, c * STEP : (c + 1) * STEP] = jnp.where(picked, nn(w_high, owns), 0.0).astype(BF16)
        comb[1, :, c * STEP : (c + 1) * STEP] = jnp.where(picked, nn(w_low, owns), 0.0).astype(BF16)

    there.wait()

    def load(n):
        block = got[pl.ds(pl.multiple_of(n * 16, 16), 16)].astype(F32)
        return block[0:8], block[8:9] + block[9:10], block[10:11] + block[11:12]

    def forward(n, state):
        held, ahead, _ = load(n)
        scanned[pl.ds(pl.multiple_of(n * 8, 8), 8)] = state
        return state * ahead + held

    def backward(n, state):
        n = NSP - 1 - n
        held, _, behind = load(n)
        first = scanned[pl.ds(pl.multiple_of(n * 8, 8), 8)]
        both = jnp.where(iota((8, W), 0) < 4, first, state)
        answers[pl.ds(pl.multiple_of(n * 16, 16), 16)] = jnp.concatenate(
            [both, jnp.zeros((8, W), F32)], axis=0
        ).astype(BF16)
        return state * behind + held

    lax.fori_loop(0, NSP, forward, jnp.zeros((8, W), F32))
    lax.fori_loop(0, NSP, backward, jnp.zeros((8, W), F32))
    again.start()
    carries[mine_s] = answers[mine_s]
    again.wait()

    i, j = iota((W, 512), 0), iota((W, 512), 1)
    spot = (i >> 2) * 16 + (i & 3)
    enter_f = nn(onehot(j == spot), carries[...]).astype(BF16)
    enter_b = nn(onehot(j == spot + 4), carries[...]).astype(BF16)
    heads = within + nt(reach_f, enter_f) + nt(reach_b, enter_b)
    mean = jnp.mean(heads * heads, axis=-1, keepdims=True)
    gate = out_gate[...].astype(F32)
    gated = heads * lax.rsqrt(mean + EPS) * head_gain[...] * (gate * jax.nn.sigmoid(gate))
    gat[y, x] = gated.astype(BF16)
    heads_all = Gather(torus, gat, T, 0, gsend, grecv, 0)
    heads_all.run()
    own[0].wait()
    own[1].wait()
    project.wait()
    total = res[...].astype(F32)
    for n in range(NTP):
        total = total + nn(gat[n // 4, n % 4], wo[n])
    stream = total.astype(BF16)

    for c in range(SLOTS // STEP):
        sent[c * 8 : (c + 1) * 8] = (
            nn(disp[c * STEP : (c + 1) * STEP, :], stream).astype(BF16).reshape(8, PAD, W)
        )
    shipped.start()
    came[pl.ds(sp, 1)] = sent[pl.ds(sp, 1)]
    shipped.wait()
    i, j = iota((4 * CAP, 4 * PAD), 0), iota((4 * CAP, 4 * PAD), 1)
    pack = (j >= 0) & False
    for n in range(4):
        pack = pack | ((i >= n * CAP) & (i < (n + 1) * CAP) & (j == i + n * (PAD - CAP)))
    pack = onehot(pack)
    i, j = iota((4 * PAD, 4 * CAP), 0), iota((4 * PAD, 4 * CAP), 1)
    unpack = (j >= 0) & False
    for n in range(4):
        unpack = unpack | ((j >= n * CAP) & (j < (n + 1) * CAP) & (i == j + n * (PAD - CAP)))
    unpack = onehot(unpack)
    for g in range(8):
        rows[y, x, g * 4 * CAP : (g + 1) * 4 * CAP, :] = nn(
            pack, came[4 * g : 4 * g + 4].reshape(4 * PAD, W)
        ).astype(BF16)
    features = Gather(torus, rows, ROWS, 0, gsend, grecv, 1)
    features.run()

    own[2].wait()
    own[3].wait()
    own[4].wait()
    down.wait()

    @pl.loop(0, ROWS // TILE)
    def _(n):
        where = pl.ds(pl.multiple_of(n * TILE, TILE), TILE)
        squares = jnp.zeros((TILE, W), F32)
        for k in range(NTP):
            block = rows[k // 4, k % 4, where].astype(F32)
            squares = squares + block * block
            xs[:, k * W : (k + 1) * W] = (block * norm_gain[k : k + 1, :]).astype(BF16)
        scale = lax.rsqrt(jnp.sum(squares, axis=-1, keepdims=True) * (1.0 / (NTP * W)) + EPS)
        gates = jnp.minimum(nn(xs[...], wg[...]) * scale, LIMIT)
        ups = jnp.clip(nn(xs[...], wu[...]) * scale, -LIMIT, LIMIT)
        act[...] = (gates * jax.nn.sigmoid(ALPHA * gates) * (ups + 1.0)).astype(BF16)
        for k in range(4):
            wide_part = nn(act[...], wd[:, k * 512 : (k + 1) * 512]).astype(BF16)
            for l in range(4):
                part[k, l, where] = wide_part[:, l * W : (l + 1) * W]

    sums = Reduce(torus, part, ROWS, 0, wide, narrow, rsend, rrecv, 0)
    sums.run()
    for g in range(8):
        outs[4 * g : 4 * g + 4] = (
            nn(unpack, part[y, x, g * 4 * CAP : (g + 1) * 4 * CAP, :]).astype(BF16).reshape(4, PAD, W)
        )
    returned.start()
    back[pl.ds(sp, 1)] = outs[pl.ds(sp, 1)]
    returned.wait()
    answer = stream.astype(F32)
    for n in range(2):
        answer = answer + nn(comb[n], back[...].reshape(SLOTS, W))
    mixed[...] = answer.astype(BF16)
    heads_all.drain()
    features.drain()
    sums.drain()


def shards(
    residual, query_in, value_in, forget_fwd, forget_bwd, jumps, gate_gap, out_gate, head_gain,
    out_weight, norm_gain, route_ids, route_weights, w_gate, w_up, w_down,
):
    vmem = pl.BlockSpec(memory_space=pltpu.VMEM)
    hbm = pl.BlockSpec(memory_space=pl.ANY)
    dma = pltpu.SemaphoreType.DMA
    buf = pltpu.VMEM
    return pl.pallas_call(
        layer,
        out_shape=jax.ShapeDtypeStruct((T, W), BF16),
        in_specs=[hbm] + [vmem] * 8 + [hbm] + [vmem] * 3 + [hbm] * 3,
        out_specs=vmem,
        scratch_shapes=[
            buf((2048, 256), BF16), buf((2048, 256), BF16), buf((256, 2048), BF16),
            buf((NTP, W, W), BF16), buf((T, W), BF16),
            buf((512, W), BF16), buf((512, W), BF16), buf((256, W), F32), buf((512, W), BF16), buf((512, W), BF16),
            buf((4, 4, T, W), BF16), buf((SLOTS, T), BF16), buf((2, T, SLOTS), BF16),
            buf((NSP, PAD, W), BF16), buf((NSP, PAD, W), BF16), buf((4, 4, ROWS, W), BF16),
            buf((TILE, 2048), BF16), buf((TILE, 256), BF16), buf((4, 4, ROWS, W), BF16),
            buf((12, 4, ROWS // 4, W), BF16), buf((12, ROWS // 4, W), BF16),
            buf((NSP, PAD, W), BF16), buf((NSP, PAD, W), BF16),
            dma((5,)), dma((4, NSP)), dma((4, NSP)), dma((2, NTP)), dma((2, NTP)),
            dma((48,)), dma((48,)), dma((24,)), dma((24,)),
        ],
        compiler_params=pltpu.CompilerParams(
            collective_id=0, has_side_effects=True, vmem_limit_bytes=60 * 1024 * 1024
        ),
    )(
        residual, query_in, value_in, forget_fwd, forget_bwd, jumps, gate_gap, out_gate,
        head_gain.reshape(1, W), out_weight, norm_gain.reshape(NTP, W), route_ids, route_weights,
        w_gate, w_up, w_down,
    )


def solution(mesh):
    return jax.shard_map(
        shards,
        mesh=mesh,
        in_specs=(
            P("sp", None), P("sp", "tp"), P("sp", "tp"), P("sp", "tp"), P("sp", "tp"), P("tp", "sp"),
            P(None, "tp"), P("sp", "tp"), P("tp"), P("tp", None), P(), P("sp", None), P("sp", None),
            P("sp", None, "tp"), P("sp", None, "tp"), P("sp", None, "tp"),
        ),
        out_specs=P("sp", "tp"),
        check_vma=False,
    )
```

```python
import jax
import jax.numpy as jnp
from jax import lax
from jax.experimental import pallas as pl
from jax.experimental.pallas import tpu as pltpu
from jax.sharding import PartitionSpec as P

MESH = pl.DeviceIdType.MESH
HIGH = lax.Precision.HIGHEST
F32 = jnp.float32
BF16 = jnp.bfloat16
NSP = 32
NTP = 16
T = 192
W = 128
CAP = 36
PAD = 48
ROWS = NSP * CAP
SLOTS = NSP * PAD
SEND = 40
CHUNKS = 4
BLOCKS = NSP // CHUNKS
TILE = BLOCKS * CAP
PLAN = (
    ("a0", 0), ("a0", 1), ("a1", 0), ("a1", 1), ("a0", 2), ("a2", 0), ("a2", 1), ("a1", 2), ("a3", 0), ("a0", 3),
    ("a2", 2), ("a1", 3), ("a4", 0), ("r0", 0), ("a3", 2), ("a2", 3), ("r1", 0), ("a3", 3), ("a3", 1), ("a4", 2),
    ("r0", 2), ("a4", 3), ("r0", 3), ("a4", 1), ("r1", 2), ("r1", 3), ("r0", 1), ("r2", 3), ("r1", 1), ("r3", 3),
    ("r2", 2), ("r2", 1), ("r4", 3), ("r3", 2), ("r2", 0), ("r3", 1), ("r4", 2), ("r3", 0), ("r4", 1), ("r4", 0),
)
EPS = 1e-06
LIMIT = 7.0
ALPHA = 1.702


def iota(shape, dim):
    return lax.broadcasted_iota(jnp.int32, shape, dim)


def nn(a, b, precision=None):
    return jnp.dot(a, b, preferred_element_type=F32, precision=precision)


def nt(a, b, precision=None):
    return lax.dot_general(a, b, (((1,), (1,)), ((), ())), preferred_element_type=F32, precision=precision)


def tn(a, b, precision=None):
    return lax.dot_general(a, b, (((0,), (0,)), ((), ())), preferred_element_type=F32, precision=precision)


def onehot(mask):
    return jnp.where(mask, 1.0, 0.0).astype(BF16)


def split(a):
    high = a.astype(BF16)
    return high, (a - high.astype(F32)).astype(BF16)


def remote(src, dst, send, recv, device):
    return pltpu.make_async_remote_copy(
        src_ref=src, dst_ref=dst, send_sem=send, recv_sem=recv, device_id=device, device_id_type=MESH
    )


def offset(n, size):
    return (n + 1) // 2 if n % 2 else (size - n // 2) % size


class Exchange:
    def __init__(self, axis, size, source, target, send, recv):
        self.axis, self.size, self.source, self.target = axis, size, source, target
        self.send, self.recv = send, recv
        self.me = lax.axis_index(axis)

    def partners(self, n):
        o = offset(n, self.size)
        return lax.rem(self.me + o, self.size), lax.rem(self.me + self.size - o, self.size)

    def out(self, n):
        to, _ = self.partners(n)
        return remote(
            self.source(n, to), self.target(n, self.me), self.send.at[n], self.recv.at[n], {self.axis: to}
        )

    def into(self, n):
        to, origin = self.partners(n)
        return remote(
            self.source(n, to), self.target(n, origin), self.send.at[n], self.recv.at[n], {self.axis: to}
        )

    def start(self, numbers):
        for n in numbers:
            self.out(n).start()

    def wait(self, numbers):
        for n in numbers:
            self.into(n).wait_recv()

    def drain(self):
        for n in range(1, self.size):
            self.out(n).wait_send()


class Opposite(Exchange):
    def partners(self, n):
        to, origin = Exchange.partners(self, n)
        return origin, to


def quarters(rows):
    first = -(-rows // 64) * 16
    return (0, first), (first, rows // 2 - first)


class Torus:
    def __init__(self):
        t = lax.axis_index("tp")
        self.y, self.x = t // 4, lax.rem(t, 4)

    def index(self, along_x):
        return self.x if along_x else self.y

    def device(self, along_x, j):
        return {"tp": self.y * 4 + j if along_x else j * 4 + self.x}


def near(i):
    return lax.rem(i + 1, 4), lax.rem(i + 3, 4), lax.rem(i + 2, 4)


class Gather:
    def __init__(self, torus, ref, rows, base, send, recv, number):
        self.t, self.ref, self.rows, self.base = torus, ref, rows, base
        self.send, self.recv, self.number = send, recv, number

    def view(self, half, stage, j, q):
        start, length = quarters(self.rows)[q]
        rows = pl.ds(self.base + half * (self.rows // 2) + start, length)
        if (half == 0) == (stage == 0):
            return self.ref.at[self.t.y, j, rows] if stage == 0 else self.ref.at[:, j, rows]
        return self.ref.at[j, self.t.x, rows] if stage == 0 else self.ref.at[j, :, rows]

    def copy(self, half, stage, k, arriving=False):
        along = (half == 0) == (stage == 0)
        i = self.t.index(along)
        p, m, f = near(i)
        up = k < 3
        to = p if up else m
        q = (0, 1, 0, 1, 0, 1)[k]
        if arriving:
            j = (m, m, f, p, p, f)[k]
        else:
            j = (i, i, m, i, i, p)[k]
        ref = self.view(half, stage, j, q)
        n = self.number * 24 + half * 12 + stage * 6 + k
        return remote(ref, ref, self.send.at[n], self.recv.at[n], self.t.device(along, to))

    def begin(self, half, stage):
        for k in (0, 3, 1, 4):
            self.copy(half, stage, k).start()

    def relay(self, half, stage):
        for k, then in ((0, 2), (3, 5)):
            self.copy(half, stage, k, True).wait_recv()
            self.copy(half, stage, then).start()

    def end(self, half, stage):
        for k in (1, 4, 2, 5):
            self.copy(half, stage, k, True).wait_recv()

    def drain(self):
        for half in range(2):
            for stage in range(2):
                for k in range(6):
                    self.copy(half, stage, k).wait_send()

    def run(self):
        for stage in range(2):
            for half in range(2):
                self.begin(half, stage)
            for half in range(2):
                self.relay(half, stage)
            for half in range(2):
                self.end(half, stage)


class Reduce:
    def __init__(self, torus, ref, rows, base, wide, narrow, send, recv, number):
        self.t, self.ref, self.rows, self.base = torus, ref, rows, base
        self.wide, self.narrow, self.send, self.recv, self.number = wide, narrow, send, recv, number

    def along(self, half, stage):
        return (half == 0) != (stage == 0)

    def view(self, half, stage, j, q):
        start, length = quarters(self.rows)[q]
        rows = pl.ds(self.base + half * (self.rows // 2) + start, length)
        if self.along(half, stage):
            return self.ref.at[self.t.y, j, rows] if stage == 1 else self.ref.at[:, j, rows]
        return self.ref.at[j, self.t.x, rows] if stage == 1 else self.ref.at[j, :, rows]

    def slot(self, half, stage, k):
        n = (self.number * 2 + half) * 6 + k
        rows = pl.ds(0, quarters(self.rows)[k % 2][1])
        return self.wide.at[n, :, rows] if stage == 0 else self.narrow.at[n, rows]

    def copy(self, half, stage, k):
        along = self.along(half, stage)
        i = self.t.index(along)
        p, m, f = near(i)
        to = p if k < 3 else m
        q = (0, 1, 0, 1, 0, 1)[k]
        j = (f, p, p, f, m, m)[k]
        n = self.number * 24 + half * 12 + stage * 6 + k
        return remote(
            self.view(half, stage, j, q),
            self.slot(half, stage, k),
            self.send.at[n],
            self.recv.at[n],
            self.t.device(along, to),
        )

    def add(self, half, stage, j, q, ks):
        own = self.view(half, stage, j, q)
        refs = [self.slot(half, stage, k) for k in ks]
        if stage == 0:
            @pl.loop(0, 4)
            def _(a):
                total = own[a].astype(F32)
                for ref in refs:
                    total = total + ref[a].astype(F32)
                own[a] = total.astype(BF16)
        else:
            total = own[...].astype(F32)
            for ref in refs:
                total = total + ref[...].astype(F32)
            own[...] = total.astype(BF16)

    def begin(self, half, stage):
        for k in (0, 3, 1, 4):
            self.copy(half, stage, k).start()

    def relay(self, half, stage):
        p, m, f = near(self.t.index(self.along(half, stage)))
        self.copy(half, stage, 0).wait_recv()
        self.add(half, stage, p, 0, (0,))
        self.copy(half, stage, 2).start()
        self.copy(half, stage, 3).wait_recv()
        self.add(half, stage, m, 1, (3,))
        self.copy(half, stage, 5).start()

    def end(self, half, stage):
        i = self.t.index(self.along(half, stage))
        for q, ks in ((0, (2, 4)), (1, (1, 5))):
            for k in ks:
                self.copy(half, stage, k).wait_recv()
            self.add(half, stage, i, q, ks)

    def drain(self):
        for half in range(2):
            for stage in range(2):
                for k in range(6):
                    self.copy(half, stage, k).wait_send()

    def run(self):
        for stage in range(2):
            for half in range(2):
                self.begin(half, stage)
            for half in range(2):
                self.relay(half, stage)
            for half in range(2):
                self.end(half, stage)


def layer(
    residual, query_in, value_in, forget_fwd, forget_bwd, jumps, gate_gap, out_gate, head_gain,
    out_weight, norm_gain, route_ids, route_weights, w_gate, w_up, w_down,
    mixed,
    wg, wu, wd, wo, res, states, got, scanned, answers, carries,
    gat, disp, comb, sent, came, rows, xs, act, part, wide, narrow, outs, back,
    local, zsend, zrecv, tsend, trecv, gsend, grecv, rsend, rrecv,
):
    sp, tp = lax.axis_index("sp"), lax.axis_index("tp")
    torus = Torus()
    y, x = torus.y, torus.x

    came[:, 32:PAD] = jnp.zeros((NSP, PAD - 32, W), BF16)
    back[:, 32:PAD] = jnp.zeros((NSP, PAD - 32, W), BF16)
    barrier = pltpu.get_barrier_semaphore()

    @pl.loop(1, NSP)
    def _(d):
        pl.semaphore_signal(barrier, 1, device_id={"sp": lax.rem(sp + d, NSP)}, device_id_type=MESH)

    @pl.loop(1, NTP)
    def _(d):
        pl.semaphore_signal(barrier, 1, device_id={"tp": lax.rem(tp + d, NTP)}, device_id_type=MESH)

    mine_t = pl.ds(pl.multiple_of(tp * W, W), W)
    own = [
        pltpu.make_async_copy(residual.at[:, mine_t], res, local.at[0]),
        pltpu.make_async_copy(out_weight.at[:, mine_t], wo.at[tp], local.at[1]),
        pltpu.make_async_copy(w_gate.at[0], wg, local.at[2]),
        pltpu.make_async_copy(w_up.at[0], wu, local.at[3]),
        pltpu.make_async_copy(
            w_down.at[0, pl.ds(pl.multiple_of(tp * 256, 256), 256)], wd.at[:, mine_t], local.at[4]
        ),
    ]
    for copy in own:
        copy.start()

    ti, si = iota((T, T), 0), iota((T, T), 1)
    until = jnp.where(si <= ti, 1.0, 0.0)
    before = jnp.where(si < ti, 1.0, 0.0)
    jump = jnp.broadcast_to(jumps[...], (8, T))
    jump_in = nt(until, jump, HIGH)[:, 0:1]
    jump_ex = nt(before, jump, HIGH)[:, 0:1]
    jump_in_row = nt(jump, until, HIGH)[0:1, :]
    jump_ex_row = nt(jump, before, HIGH)[0:1, :]
    jump_all = jump_in_row[:, T - 1 : T]

    raw = query_in[...].astype(F32)
    queries = raw * jax.nn.sigmoid(raw)
    values = value_in[...]

    key_f = gate_gap[0:1, :] * jax.nn.sigmoid(-forget_fwd[...].astype(F32))
    log_f = jnp.log1p(-key_f)
    sum_f = nn(until, log_f, HIGH)
    all_f = sum_f[T - 1 : T, :]
    mid_f = all_f * 0.5
    decay_f = jnp.exp(all_f + jump_all)
    state_f = tn(values, (key_f * jnp.exp((all_f - sum_f) + (jump_all - jump_in))).astype(BF16))
    reach_f = (queries * jnp.exp(sum_f + jump_in)).astype(BF16)

    key_b = gate_gap[1:2, :] * jax.nn.sigmoid(-forget_bwd[...].astype(F32))
    log_b = jnp.log1p(-key_b)
    sum_b = nn(before, log_b, HIGH)
    all_b = sum_b[T - 1 : T, :] + log_b[T - 1 : T, :]
    mid_b = all_b * 0.5
    decay_b = jnp.exp(all_b + jump_all)
    state_b = tn(values, (key_b * jnp.exp(sum_b + jump_ex)).astype(BF16))
    reach_b = (queries * jnp.exp((all_b - sum_b) + (jump_all - jump_ex))).astype(BF16)

    i, j = iota((512, 256), 0), iota((512, 256), 1)
    r = i & 15
    place = onehot(((r < 8) & (j == (i >> 4) * 4 + (r & 3) + jnp.where(r < 4, 0, 128))))
    pieces = nn(place, jnp.concatenate([state_f.astype(BF16), state_b.astype(BF16)], axis=0))
    r = iota((512, W), 0) & 15
    for number, decay in ((8, decay_f), (10, decay_b)):
        high, low = split(decay)
        pieces = jnp.where(r == number, high.astype(F32), pieces)
        pieces = jnp.where(r == number + 1, low.astype(F32), pieces)
    states[...] = pieces.astype(BF16)

    pl.semaphore_wait(barrier, NSP + NTP - 2)

    def part16(ref, n):
        return ref.at[pl.ds(pl.multiple_of(n * 16, 16), 16)]

    def slab(ref, n):
        return ref.at[n, pl.ds(0, SEND)]

    there = Exchange(
        "sp", NSP, lambda n, to: part16(states, to), lambda n, me: part16(got, me), zsend.at[0], zrecv.at[0]
    )
    again = Exchange(
        "sp", NSP, lambda n, to: part16(answers, to), lambda n, me: part16(carries, me), zsend.at[1], zrecv.at[1]
    )
    shipped = Exchange(
        "sp", NSP, lambda n, to: slab(sent, to), lambda n, me: slab(came, n), zsend.at[2], zrecv.at[2]
    )
    returned = Opposite(
        "sp", NSP, lambda n, to: slab(outs, n), lambda n, me: slab(back, me), zsend.at[3], zrecv.at[3]
    )
    project = Exchange(
        "tp", NTP, lambda n, to: out_weight.at[:, pl.ds(pl.multiple_of(to * W, W), W)],
        lambda n, me: wo.at[me], tsend.at[0], trecv.at[0],
    )
    down = Exchange(
        "tp", NTP, lambda n, to: w_down.at[0, pl.ds(pl.multiple_of(to * 256, 256), 256)],
        lambda n, me: wd.at[:, pl.ds(pl.multiple_of(me * W, W), W)], tsend.at[1], trecv.at[1],
    )
    far_first = tuple(range(NSP - 1, 0, -1))
    there.start(far_first)
    project.start(range(1, NTP))
    down.start(range(1, NTP))
    mine_s = pl.ds(pl.multiple_of(sp * 16, 16), 16)
    got[mine_s] = states[mine_s]

    scores = jnp.where(
        si <= ti,
        nt((queries * jnp.exp(sum_f - mid_f)).astype(BF16), (key_f * jnp.exp(mid_f - sum_f)).astype(BF16))
        * jnp.exp(jnp.minimum(jump_in - jump_in_row, 0.0)),
        0.0,
    )
    scores = scores + jnp.where(
        si >= ti,
        nt((queries * jnp.exp(mid_b - sum_b)).astype(BF16), (key_b * jnp.exp(sum_b - mid_b)).astype(BF16))
        * jnp.exp(jnp.minimum(jump_ex_row - jump_ex, 0.0)),
        0.0,
    )
    within = nn(scores.astype(BF16), values)

    ids = route_ids[...]
    weights = route_weights[...]
    line = iota((W, T), 0)
    named = jnp.zeros((W, T), F32)
    weighted = jnp.zeros((W, T), F32)
    for n in range(4):
        hit = ids[n : n + 1, :] == line
        named = named + jnp.where(hit, 1.0, 0.0)
        weighted = weighted + jnp.where(hit, weights[n : n + 1, :], 0.0)
    named, weighted = named.T, weighted.T
    named16 = named.astype(BF16)
    rank16 = nn(before.astype(BF16), named16).astype(BF16)
    w_high, w_low = split(weighted)
    STEP = 384
    for c in range(SLOTS // STEP):
        slot, e = iota((STEP, W), 0) + c * STEP, iota((STEP, W), 1)
        owns = onehot((slot >= e * PAD) & (slot < e * PAD + PAD))
        number = nt(owns, jnp.broadcast_to(lax.broadcasted_iota(jnp.int32, (8, W), 1).astype(F32), (8, W)).astype(BF16))
        turn = (iota((STEP, 1), 0) + c * STEP).astype(F32) - PAD * number[:, 0:1]
        picked = (nt(owns, named16) > 0.5) & (nt(owns, rank16) == turn)
        disp[c * STEP : (c + 1) * STEP, :] = onehot(picked)

        slot, e = iota((W, STEP), 1) + c * STEP, iota((W, STEP), 0)
        owns = onehot((slot >= e * PAD) & (slot < e * PAD + PAD))
        number = nn(lax.broadcasted_iota(jnp.int32, (8, W), 1).astype(F32).astype(BF16), owns)
        turn = (iota((1, STEP), 1) + c * STEP).astype(F32) - PAD * number[0:1, :]
        picked = (nn(named16, owns) > 0.5) & (nn(rank16, owns) == turn)
        comb[0, :, c * STEP : (c + 1) * STEP] = jnp.where(picked, nn(w_high, owns), 0.0).astype(BF16)
        comb[1, :, c * STEP : (c + 1) * STEP] = jnp.where(picked, nn(w_low, owns), 0.0).astype(BF16)

    there.wait(range(1, NSP))

    def load(n):
        block = got[pl.ds(pl.multiple_of(n * 16, 16), 16)].astype(F32)
        return block[0:8], block[8:9] + block[9:10], block[10:11] + block[11:12]

    def forward(n, state):
        held, ahead, _ = load(n)
        scanned[pl.ds(pl.multiple_of(n * 8, 8), 8)] = state
        return state * ahead + held

    def backward(n, state):
        n = NSP - 1 - n
        held, _, behind = load(n)
        first = scanned[pl.ds(pl.multiple_of(n * 8, 8), 8)]
        both = jnp.where(iota((8, W), 0) < 4, first, state)
        answers[pl.ds(pl.multiple_of(n * 16, 16), 16)] = jnp.concatenate(
            [both, jnp.zeros((8, W), F32)], axis=0
        ).astype(BF16)
        return state * behind + held

    lax.fori_loop(0, NSP, forward, jnp.zeros((8, W), F32))
    lax.fori_loop(0, NSP, backward, jnp.zeros((8, W), F32))
    again.start(far_first)
    carries[mine_s] = answers[mine_s]
    again.wait(range(1, NSP))

    i, j = iota((W, 512), 0), iota((W, 512), 1)
    spot = (i >> 2) * 16 + (i & 3)
    enter_f = nn(onehot(j == spot), carries[...]).astype(BF16)
    enter_b = nn(onehot(j == spot + 4), carries[...]).astype(BF16)
    heads = within + nt(reach_f, enter_f) + nt(reach_b, enter_b)
    mean = jnp.mean(heads * heads, axis=-1, keepdims=True)
    gate = out_gate[...].astype(F32)
    gated = heads * lax.rsqrt(mean + EPS) * head_gain[...] * (gate * jax.nn.sigmoid(gate))
    gat[y, x] = gated.astype(BF16)
    heads_all = Gather(torus, gat, T, 0, gsend, grecv, 0)
    heads_all.run()
    own[0].wait()
    own[1].wait()
    project.wait(range(1, NTP))
    total = res[...].astype(F32)
    for n in range(NTP):
        total = total + nn(gat[n // 4, n % 4], wo[n])
    stream = total.astype(BF16)

    for c in range(SLOTS // STEP):
        sent[c * 8 : (c + 1) * 8] = (
            nn(disp[c * STEP : (c + 1) * STEP, :], stream).astype(BF16).reshape(8, PAD, W)
        )
    def blocks(c):
        return [n for n in range(c * BLOCKS, (c + 1) * BLOCKS) if n]

    for c in range(CHUNKS):
        shipped.start(blocks(c))
    came[0:1] = sent[pl.ds(sp, 1)]
    i, j = iota((4 * CAP, 4 * PAD), 0), iota((4 * CAP, 4 * PAD), 1)
    pack = (j >= 0) & False
    for n in range(4):
        pack = pack | ((i >= n * CAP) & (i < (n + 1) * CAP) & (j == i + n * (PAD - CAP)))
    pack = onehot(pack)
    i, j = iota((4 * PAD, 4 * CAP), 0), iota((4 * PAD, 4 * CAP), 1)
    unpack = (j >= 0) & False
    for n in range(4):
        unpack = unpack | ((j >= n * CAP) & (j < (n + 1) * CAP) & (i == j + n * (PAD - CAP)))
    unpack = onehot(unpack)
    features = [Gather(torus, rows, TILE, c * TILE, gsend, grecv, 1 + c) for c in range(CHUNKS)]
    sums = [Reduce(torus, part, TILE, c * TILE, wide, narrow, rsend, rrecv, c) for c in range(CHUNKS)]

    def each(step, *args):
        for half in range(2):
            step(half, *args)

    def arrive(c):
        shipped.wait(blocks(c))
        for g in range(c * BLOCKS // 4, (c + 1) * BLOCKS // 4):
            rows[y, x, g * 4 * CAP : (g + 1) * 4 * CAP, :] = nn(
                pack, came[4 * g : 4 * g + 4].reshape(4 * PAD, W)
            ).astype(BF16)

    def compute(c):
        where = slice(c * TILE, (c + 1) * TILE)
        squares = jnp.zeros((TILE, W), F32)
        for k in range(NTP):
            block = rows[k // 4, k % 4, where].astype(F32)
            squares = squares + block * block
            xs[:, k * W : (k + 1) * W] = (block * norm_gain[k : k + 1, :]).astype(BF16)
        scale = lax.rsqrt(jnp.sum(squares, axis=-1, keepdims=True) * (1.0 / (NTP * W)) + EPS)
        gates = jnp.minimum(nn(xs[...], wg[...]) * scale, LIMIT)
        ups = jnp.clip(nn(xs[...], wu[...]) * scale, -LIMIT, LIMIT)
        act[...] = (gates * jax.nn.sigmoid(ALPHA * gates) * (ups + 1.0)).astype(BF16)
        for k in range(4):
            wide_part = nn(act[...], wd[:, k * 512 : (k + 1) * 512]).astype(BF16)
            for l in range(4):
                part[k, l, where] = wide_part[:, l * W : (l + 1) * W]

    def leave(c):
        for g in range(c * BLOCKS // 4, (c + 1) * BLOCKS // 4):
            outs[4 * g : 4 * g + 4] = (
                nn(unpack, part[y, x, g * 4 * CAP : (g + 1) * 4 * CAP, :]).astype(BF16).reshape(4, PAD, W)
            )
        returned.start(blocks(c))

    def a0(c):
        arrive(c)
        each(features[c].begin, 0)

    def a1(c):
        each(features[c].relay, 0)

    def a2(c):
        for half in range(2):
            features[c].end(half, 0)
            features[c].begin(half, 1)

    def a3(c):
        each(features[c].relay, 1)

    def a4(c):
        each(features[c].end, 1)

    def r0(c):
        if ("r0", c) == first:
            own[2].wait()
            own[3].wait()
            own[4].wait()
            down.wait(range(1, NTP))
        compute(c)
        each(sums[c].begin, 0)

    def r1(c):
        each(sums[c].relay, 0)

    def r2(c):
        for half in range(2):
            sums[c].end(half, 0)
            sums[c].begin(half, 1)

    def r3(c):
        each(sums[c].relay, 1)

    def r4(c):
        each(sums[c].end, 1)
        leave(c)

    steps = dict(a0=a0, a1=a1, a2=a2, a3=a3, a4=a4, r0=r0, r1=r1, r2=r2, r3=r3, r4=r4)
    first = next(item for item in PLAN if item[0] == "r0")
    for name, c in PLAN:
        steps[name](c)
    back[pl.ds(sp, 1)] = outs[0:1]
    returned.wait(range(1, NSP))
    answer = stream.astype(F32)
    for n in range(2):
        answer = answer + nn(comb[n], back[...].reshape(SLOTS, W))
    mixed[...] = answer.astype(BF16)
    heads_all.drain()
    for c in range(CHUNKS):
        features[c].drain()
        sums[c].drain()
    for each_one in (there, again, shipped, returned, project, down):
        each_one.drain()


def shards(
    residual, query_in, value_in, forget_fwd, forget_bwd, jumps, gate_gap, out_gate, head_gain,
    out_weight, norm_gain, route_ids, route_weights, w_gate, w_up, w_down,
):
    vmem = pl.BlockSpec(memory_space=pltpu.VMEM)
    hbm = pl.BlockSpec(memory_space=pl.ANY)
    dma = pltpu.SemaphoreType.DMA
    buf = pltpu.VMEM
    return pl.pallas_call(
        layer,
        out_shape=jax.ShapeDtypeStruct((T, W), BF16),
        in_specs=[hbm] + [vmem] * 8 + [hbm] + [vmem] * 3 + [hbm] * 3,
        out_specs=vmem,
        scratch_shapes=[
            buf((2048, 256), BF16), buf((2048, 256), BF16), buf((256, 2048), BF16),
            buf((NTP, W, W), BF16), buf((T, W), BF16),
            buf((512, W), BF16), buf((512, W), BF16), buf((256, W), F32), buf((512, W), BF16), buf((512, W), BF16),
            buf((4, 4, T, W), BF16), buf((SLOTS, T), BF16), buf((2, T, SLOTS), BF16),
            buf((NSP, PAD, W), BF16), buf((NSP, PAD, W), BF16), buf((4, 4, ROWS, W), BF16),
            buf((TILE, 2048), BF16), buf((TILE, 256), BF16), buf((4, 4, ROWS, W), BF16),
            buf((12 * CHUNKS, 4, 80, W), BF16), buf((12 * CHUNKS, 80, W), BF16),
            buf((NSP, PAD, W), BF16), buf((NSP, PAD, W), BF16),
            dma((5,)), dma((4, NSP)), dma((4, NSP)), dma((2, NTP)), dma((2, NTP)),
            dma((24 + 24 * CHUNKS,)), dma((24 + 24 * CHUNKS,)), dma((24 * CHUNKS,)), dma((24 * CHUNKS,)),
        ],
        compiler_params=pltpu.CompilerParams(
            collective_id=0, has_side_effects=True, vmem_limit_bytes=60 * 1024 * 1024
        ),
    )(
        residual, query_in, value_in, forget_fwd, forget_bwd, jumps, gate_gap, out_gate,
        head_gain.reshape(1, W), out_weight, norm_gain.reshape(NTP, W), route_ids.T, route_weights.T,
        w_gate, w_up, w_down,
    )


def solution(mesh):
    return jax.shard_map(
        shards,
        mesh=mesh,
        in_specs=(
            P("sp", None), P("sp", "tp"), P("sp", "tp"), P("sp", "tp"), P("sp", "tp"), P("tp", "sp"),
            P(None, "tp"), P("sp", "tp"), P("tp"), P("tp", None), P(), P("sp", None), P("sp", None),
            P("sp", None, "tp"), P("sp", None, "tp"), P("sp", None, "tp"),
        ),
        out_specs=P("sp", "tp"),
        check_vma=False,
    )
```
